32 devices in a mesh: sp: 4 (over y, x), tp: 8 (over z, core).
Axes of the slice: x: 2, y: 2, z: 4, core: 2. Of those that a mesh axis runs over, the one named last changes fastest.
Arguments:
- tokens: bfloat16 [8, 3072, 2048], P(None, ('sp', 'tp')), may hold values from -13 to 13
- in_gain: float32 [2048], replicated, may hold values from 0.1 to 1.9
- w_key: bfloat16 [2048, 512], P('tp'), may hold values from -0.125 to 0.125
- w_value: bfloat16 [2048, 512], P('tp'), may hold values from -0.125 to 0.125
- k_gain: float32 [128], replicated, may hold values from 0.1 to 1.9
- new_query: bfloat16 [8, 1024], replicated, may hold values from -6 to 6
- q_gain: float32 [128], replicated, may hold values from 0.1 to 1.9
- stick_bias: float32 [8], replicated, may hold values from -13 to -3
Outputs:
- key_cache: bfloat16 [32, 3072, 128], P('tp', 'sp')
- value_cache: bfloat16 [32, 3072, 128], P('tp', 'sp')
- read_out: float32 [32, 256], P('tp')
The draws below stay inside these ranges and needn't reach their ends.
All inputs are finite; a program needn't handle non-finite values.
Results may differ from the reference program's by a relative error of at most 0.005.
Values may be sent and summed in bfloat16 or wider, within the bound.
A program may use at most 64 MiB of HBM per device.

```python
import jax
import jax.numpy as jnp
from jax import lax

D = 2048
HEADS = 8
KVH = 4
HD = 128
SEQS = 8
LENGTH = 3072


def draw_tokens(key, part):
    noise_key, common_key, level_key = jax.random.split(jax.random.fold_in(key, 11), 3)
    block_count = LENGTH // 32
    noise_part = jnp.clip(jax.random.normal(noise_key, (SEQS, LENGTH, D), jnp.float32), -5.0, 5.0)
    levels = jnp.exp(jax.random.uniform(level_key, (SEQS, block_count, 1), jnp.float32, -1.2, 0.9))
    common = jnp.clip(jax.random.normal(common_key, (SEQS, 1, D), jnp.float32), -3.0, 3.0)
    levels = jnp.repeat(levels, 32, axis=1)
    return (noise_part + levels * common).astype(jnp.bfloat16)


def draw_stick_bias(key, part):
    order_key, fast_key, slow_key = jax.random.split(jax.random.fold_in(key, 23), 3)
    chain = jnp.log(jnp.float32(LENGTH))
    slow_bias = -chain + jax.random.uniform(slow_key, (HEADS,), jnp.float32, -1.5, 0.0)
    fast_bias = jax.random.uniform(fast_key, (HEADS,), jnp.float32, -4.5, -3.5)
    ranking = jax.random.permutation(order_key, HEADS)
    is_fast = ranking < HEADS // 2
    return jnp.where(is_fast, fast_bias, slow_bias)


def steps_of(own_key, shape, pieces, least, high):
    loudness = 1.0
    for axis_at, parts in pieces:
        heights = jax.random.uniform(jax.random.fold_in(jax.random.fold_in(own_key, 6), axis_at), (parts,), jnp.float32, least / len(pieces), high / len(pieces))
        loudness = loudness * jnp.repeat(jnp.exp(heights), shape[axis_at] // parts).reshape((-1,) + (1,) * (len(shape) - 1 - axis_at))
    return loudness


def bell_draw(rng, dims, deviation, reach, pieces=(), dtype=jnp.bfloat16):
    loudness = steps_of(rng, dims, pieces, -0.22, 0.18) if pieces else 1.0
    result = jax.random.normal(rng, dims, jnp.float32) * deviation * loudness
    return jnp.minimum(jnp.maximum(result, -reach), reach).astype(dtype)


def setup_inputs(seed: int = 0) -> dict:
    streams_of = jax.random.split(jax.random.key(seed), 9)
    return {
        "tokens": draw_tokens(jax.random.fold_in(streams_of[8], 71), 0),
        "in_gain": jnp.clip(1.0 + 0.18 * jax.random.normal(streams_of[1], (D,), jnp.float32), 0.1, 1.9),
        "w_key": bell_draw(streams_of[2], (D, KVH * HD), D ** -0.5, 0.125, ((0, 8),)),
        "w_value": bell_draw(streams_of[3], (D, KVH * HD), D ** -0.5, 0.125, ((0, 8),)),
        "k_gain": jnp.clip(1.0 + 0.18 * jax.random.normal(streams_of[4], (HD,), jnp.float32), 0.1, 1.9),
        "new_query": bell_draw(streams_of[5], (SEQS, HEADS * HD), 1.0, 6.0),
        "q_gain": jnp.clip(1.0 + 0.18 * jax.random.normal(streams_of[6], (HD,), jnp.float32), 0.1, 1.9),
        "stick_bias": draw_stick_bias(jax.random.fold_in(streams_of[8], 71), 0),
    }


NORM_EPS = 1e-06

def root_norm(values, scaling):
    inverse = lax.rsqrt(lax.optimization_barrier(jnp.mean(values * values, axis=-1, keepdims=True)) + NORM_EPS)
    return values * inverse * scaling

def reference(tokens, in_gain, w_key, w_value, k_gain, new_query, q_gain, stick_bias):
    per_group = HEADS // KVH
    query_rows = root_norm(new_query.astype(jnp.float32).reshape(SEQS, KVH, per_group, HD), q_gain).astype(jnp.bfloat16)
    bias_rows = stick_bias.astype(jnp.float32).reshape(KVH, per_group)

    def per_sequence(inputs):
        seq_tokens, seq_query = inputs
        normed = root_norm(seq_tokens.astype(jnp.float32), in_gain).astype(jnp.bfloat16)
        key_raw = jnp.dot(normed, w_key, preferred_element_type=jnp.float32).reshape(LENGTH, KVH, HD)
        key_rows = root_norm(key_raw, k_gain).astype(jnp.bfloat16)
        value_rows = jnp.dot(normed, w_value, preferred_element_type=jnp.float32).astype(jnp.bfloat16).reshape(LENGTH, KVH, HD)
        scores = jnp.einsum('hqe,phe->hqp', seq_query.astype(jnp.float32), key_rows.astype(jnp.float32)) * HD ** (-0.5) + bias_rows[:, :, None]
        log_keep = jax.nn.log_sigmoid(-scores)
        log_after = lax.cumsum(log_keep, axis=2, reverse=True) - log_keep
        weights = jnp.exp(jax.nn.log_sigmoid(scores) + log_after).astype(jnp.bfloat16)
        read_rows = jnp.einsum('hqp,phe->hqe', weights.astype(jnp.float32), value_rows.astype(jnp.float32))
        return (key_rows.transpose(1, 0, 2), value_rows.transpose(1, 0, 2), read_rows.reshape(KVH, per_group * HD))
    key_all, value_all, read_all = lax.map(per_sequence, (tokens, query_rows))
    key_cache = key_all.transpose(1, 0, 2, 3).reshape(KVH * SEQS, LENGTH, HD)
    value_cache = value_all.transpose(1, 0, 2, 3).reshape(KVH * SEQS, LENGTH, HD)
    read_out = read_all.transpose(1, 0, 2).reshape(KVH * SEQS, per_group * HD)
    return (key_cache, value_cache, read_out)
```

```python
import functools

import jax
import jax.numpy as jnp
from jax import lax
from jax.experimental import pallas as pl
from jax.experimental.pallas import tpu as pltpu
from jax.sharding import PartitionSpec as P

NORM_EPS = 1e-06
MESH = pl.DeviceIdType.MESH
CORES = 2
SUBLANES = 16


def root_norm(values, scaling):
    inverse = lax.rsqrt(jnp.mean(values * values, axis=-1, keepdims=True) + NORM_EPS)
    return values * inverse * scaling


def remote(src, dst, send, recv, sp, tp):
    return pltpu.make_async_remote_copy(
        src_ref=src, dst_ref=dst, send_sem=send, recv_sem=recv, device_id=(sp, tp), device_id_type=MESH
    )


def kernel(
    dims,
    tok_hbm, gain_ref, wk_hbm, wv_hbm, kgain_ref, query_ref, bias_ref,
    kc_hbm, vc_hbm, read_ref,
    tok, normed, wbuf, kbuf, vbuf, krecv, vrecv, parts,
    tok_sem, own_sem, p1_send, p1_recv, p2_send, p2_recv, p3_send, p3_recv,
    a_send, a_recv, mine_sem, out_sem, f_send, f_recv,
):
    nsp, ntp, heads, q, group_rows, per_group = dims
    sp, tp = lax.axis_index("sp"), lax.axis_index("tp")
    nz = ntp // CORES
    z, c = tp // CORES, tp % CORES
    partner = z * CORES + (1 - c)
    base, i = (sp // q) * q, sp % q
    seqs, tok_seq, width = tok.shape
    rows = wk_hbm.shape[0]
    part = rows // q
    hd = kc_hbm.shape[2]
    span = ntp * tok_seq
    tp_head = ntp // heads
    half = heads // 2

    def head_at(zc, j):
        home = (zc * CORES) // tp_head
        side = (home // half + (1 if j < half else 0)) % 2
        return side * half + (home % half + (half - 1 - j % half)) % half

    fetch = pltpu.make_async_copy(tok_hbm, tok, tok_sem)
    own = []
    for j in range(heads):
        h = head_at(z, j)
        cols = pl.ds(pl.multiple_of(h * hd, hd), hd)
        for n, w in enumerate((wk_hbm, wv_hbm)):
            copy = pltpu.make_async_copy(
                w.at[:, cols], wbuf.at[h, z, c, :, pl.ds(n * hd, hd)], own_sem.at[j, n]
            )
            copy.start()
            own.append(copy)
    fetch.start()

    barrier = pltpu.get_barrier_semaphore()
    for d in range(1, ntp):
        pl.semaphore_signal(barrier, inc=1, device_id=(sp, (tp + d) % ntp), device_id_type=MESH)
    for d in range(1, nsp):
        pl.semaphore_signal(barrier, inc=1, device_id=((sp + d) % nsp, tp), device_id_type=MESH)
    for copy in own:
        copy.wait()
    pl.semaphore_wait(barrier, ntp + nsp - 2)

    mine = pl.ds(pl.multiple_of(i * part, part), part)
    sends = []

    for j in range(heads):
        for d in range(1, nz):
            zt = (z + d) % nz
            h = head_at(zt, j)
            block = wbuf.at[h, z, c, mine]
            copy = remote(block, block, p1_send.at[j, d], p1_recv.at[j, z], sp, zt * CORES + c)
            copy.start()
            sends.append(copy)

    fetch.wait()
    step_rows = SUBLANES
    per_seq = tok_seq // step_rows

    def norm_rows(n, carry):
        s, at = n // per_seq, pl.ds(pl.multiple_of((n % per_seq) * step_rows, step_rows), step_rows)
        values = tok[s, at].astype(jnp.float32)
        normed[s, at] = root_norm(values, gain_ref[...]).astype(jnp.bfloat16)
        return carry

    lax.fori_loop(0, seqs * per_seq, norm_rows, 0)

    def spread(j):
        h = head_at(z, j)
        for d in range(1, nz):
            zs = (z + nz - d) % nz
            block = wbuf.at[h, zs, c, mine]
            remote(block, block, p1_send.at[j, d], p1_recv.at[j, zs], sp, zs * CORES + c).wait_recv()
            for e in range(1, q):
                copy = remote(
                    block, block, p2_send.at[j, e, d], p2_recv.at[j, i, zs], base + (i + e) % q, tp
                )
                copy.start()
                sends.append(copy)

    def share(j):
        h = head_at(z, j)
        for d in range(1, nz):
            zs = (z + nz - d) % nz
            for e in range(1, q):
                source = (i + e) % q
                block = wbuf.at[h, zs, c, pl.ds(pl.multiple_of(source * part, part), part)]
                remote(
                    block, block, p2_send.at[j, e, d], p2_recv.at[j, source, zs], base + source, tp
                ).wait_recv()
        block = wbuf.at[h, :, c]
        copy = remote(block, block, p3_send.at[j], p3_recv.at[j], sp, partner)
        copy.start()
        sends.append(copy)

    tile = seqs // 2

    def project(j):
        h = head_at(z, j)
        block = wbuf.at[h, :, 1 - c]
        remote(block, block, p3_send.at[j], p3_recv.at[j], sp, partner).wait_recv()

        def rows_of(n, carry):
            at = pl.ds(n * tile, tile)
            both = jnp.dot(
                normed[at].reshape(tile * tok_seq, width),
                wbuf[h].reshape(width, 2 * hd),
                preferred_element_type=jnp.float32,
            )
            key = root_norm(both[:, :hd], kgain_ref[...])
            kbuf[h, at] = key.astype(jnp.bfloat16).reshape(tile, tok_seq, hd)
            vbuf[h, at] = both[:, hd:].astype(jnp.bfloat16).reshape(tile, tok_seq, hd)
            return carry

        lax.fori_loop(0, seqs // tile, rows_of, 0)

    here = pl.ds(pl.multiple_of(tp * tok_seq, tok_seq), tok_seq)

    def deliver(j):
        h = head_at(z, j)
        for u in range(tp_head):
            target = h * tp_head + u
            at = pl.ds(u * group_rows, group_rows)

            def send(target=target, at=at):
                for n, (src, dst) in enumerate(((kbuf, krecv), (vbuf, vrecv))):
                    remote(
                        src.at[h, at], dst.at[:, here], a_send.at[n, target], a_recv.at[n, tp], sp, target
                    ).start()

            if j < heads - 1:
                send()
            else:

                @pl.when(target != tp)
                def _():
                    send()

                @pl.when(target == tp)
                def _():
                    for n, (src, dst) in enumerate(((kbuf, krecv), (vbuf, vrecv))):
                        pltpu.make_async_copy(src.at[h, at], dst.at[:, here], mine_sem.at[n]).start()

    spread(0)
    for j in range(heads):
        if j + 1 < heads:
            spread(j + 1)
        share(j)
        project(j)
        deliver(j)

    first = pl.ds(0, group_rows)
    for n, (src, dst) in enumerate(((kbuf, krecv), (vbuf, vrecv))):
        pltpu.make_async_copy(src.at[0, first], dst.at[:, here], mine_sem.at[n]).wait()
    for d in range(1, ntp):
        source = (tp + d) % ntp
        at = pl.ds(pl.multiple_of(source * tok_seq, tok_seq), tok_seq)
        for n, (src, dst) in enumerate(((kbuf, krecv), (vbuf, vrecv))):
            remote(
                src.at[0, first], dst.at[:, at], a_send.at[n, source], a_recv.at[n, source], sp, source
            ).wait_recv()
    outs = (
        pltpu.make_async_copy(krecv, kc_hbm, out_sem.at[0]),
        pltpu.make_async_copy(vrecv, vc_hbm, out_sem.at[1]),
    )
    for copy in outs:
        copy.start()

    lines = query_ref.shape[0]
    line = lax.broadcasted_iota(jnp.int32, (lines, 1), 0) // per_group
    raw = jnp.zeros((lines, span), jnp.float32)
    for r in range(group_rows):
        dots = lax.dot_general(
            query_ref[...], krecv[r], (((1,), (1,)), ((), ())), preferred_element_type=jnp.float32
        )
        raw = jnp.where(line == r, dots, raw)
    scores = raw * hd ** (-0.5) + bias_ref[...][:, :1]
    soft = jnp.log1p(jnp.exp(-jnp.abs(scores)))
    keep = -jnp.maximum(scores, 0.0) - soft
    take = jnp.minimum(scores, 0.0) - soft
    place = lax.broadcasted_iota(jnp.int32, (lines, span), 1)
    total = keep
    reach = 1
    while reach < span:
        moved = pltpu.roll(total, span - reach, 1)
        total = total + jnp.where(place < span - reach, moved, 0.0)
        reach *= 2
    weights = jnp.exp(take + (total - keep)).astype(jnp.bfloat16)
    value = jnp.zeros((lines, hd), jnp.float32)
    for r in range(group_rows):
        dots = jnp.dot(weights, vrecv[r], preferred_element_type=jnp.float32)
        value = jnp.where(line == r, dots, value)
    parts[sp, :, :hd] = value
    parts[sp, :, hd:] = jnp.broadcast_to(total[:, :1], (lines, hd))
    for d in range(1, nsp):
        copy = remote(
            parts.at[sp], parts.at[sp], f_send.at[d], f_recv.at[sp], (sp + d) % nsp, tp
        )
        copy.start()
        sends.append(copy)
    for d in range(1, nsp):
        source = (sp + d) % nsp
        remote(parts.at[source], parts.at[source], f_send.at[d], f_recv.at[source], source, tp).wait_recv()
    result = jnp.zeros((lines, hd), jnp.float32)
    later = jnp.zeros((lines, hd), jnp.float32)
    for n in reversed(range(nsp)):
        result = result + jnp.exp(later) * parts[n, :, :hd]
        later = later + parts[n, :, hd:]
    read_ref[...] = result

    for copy in sends:
        copy.wait_send()
    for d in range(1, ntp):
        target = (tp + d) % ntp
        for n, (src, dst) in enumerate(((kbuf, krecv), (vbuf, vrecv))):
            remote(
                src.at[0, first], dst.at[:, here], a_send.at[n, target], a_recv.at[n, tp], sp, target
            ).wait_send()
    for copy in outs:
        copy.wait()


def shards(sizes, tokens, in_gain, w_key, w_value, k_gain, new_query, q_gain, stick_bias):
    nsp, ntp = sizes
    seqs, tok_seq, width = tokens.shape
    rows, kv_width = w_key.shape
    hd = k_gain.shape[0]
    heads = kv_width // hd
    per_group = stick_bias.shape[0] // heads
    group_rows = heads * seqs // ntp
    used = group_rows * per_group
    lines = -(-used // 8) * 8
    nz = ntp // CORES
    q = min(nsp, rows // SUBLANES)
    query = root_norm(
        new_query.astype(jnp.float32).reshape(seqs, heads, per_group, hd), q_gain
    ).astype(jnp.bfloat16)
    query = query.transpose(1, 0, 2, 3).reshape(heads * seqs * per_group, hd)
    start = lax.axis_index("tp") * used
    query = lax.dynamic_slice_in_dim(query, start, used, 0)
    bias = jnp.broadcast_to(stick_bias.reshape(heads, 1, per_group, 1), (heads, seqs, per_group, hd))
    bias = lax.dynamic_slice_in_dim(bias.reshape(heads * seqs * per_group, hd), start, used, 0)
    if lines > used:
        query = jnp.pad(query, ((0, lines - used), (0, 0)))
        bias = jnp.pad(bias, ((0, lines - used), (0, 0)))
    span = ntp * tok_seq
    dma = pltpu.SemaphoreType.DMA
    anywhere = pl.BlockSpec(memory_space=pl.ANY)
    vmem = pl.BlockSpec(memory_space=pltpu.VMEM)
    cache = jax.ShapeDtypeStruct((group_rows, span, hd), jnp.bfloat16)
    key_cache, value_cache, read = pl.pallas_call(
        functools.partial(kernel, (nsp, ntp, heads, q, group_rows, per_group)),
        out_shape=(cache, cache, jax.ShapeDtypeStruct((lines, hd), jnp.float32)),
        in_specs=[anywhere, vmem, anywhere, anywhere, vmem, vmem, vmem],
        out_specs=(anywhere, anywhere, vmem),
        scratch_shapes=[
            pltpu.VMEM((seqs, tok_seq, width), jnp.bfloat16),
            pltpu.VMEM((seqs, tok_seq, width), jnp.bfloat16),
            pltpu.VMEM((heads, nz, CORES, rows, 2 * hd), jnp.bfloat16),
            pltpu.VMEM((heads, seqs, tok_seq, hd), jnp.bfloat16),
            pltpu.VMEM((heads, seqs, tok_seq, hd), jnp.bfloat16),
            pltpu.VMEM((group_rows, span, hd), jnp.bfloat16),
            pltpu.VMEM((group_rows, span, hd), jnp.bfloat16),
            pltpu.VMEM((nsp, lines, 2 * hd), jnp.float32),
            dma,
            dma((heads, 2)),
            dma((heads, nz)),
            dma((heads, nz)),
            dma((heads, q, nz)),
            dma((heads, q, nz)),
            dma((heads,)),
            dma((heads,)),
            dma((2, ntp)),
            dma((2, ntp)),
            dma((2,)),
            dma((2,)),
            dma((nsp,)),
            dma((nsp,)),
        ],
        compiler_params=pltpu.CompilerParams(
            collective_id=0, has_side_effects=True, vmem_limit_bytes=56 * 1024 * 1024
        ),
    )(tokens, in_gain.reshape(1, width), w_key, w_value, k_gain.reshape(1, hd), query, bias)
    return key_cache, value_cache, read[:used].reshape(group_rows, per_group * hd)


def solution(mesh):
    return jax.shard_map(
        functools.partial(shards, (mesh.shape["sp"], mesh.shape["tp"])),
        mesh=mesh,
        in_specs=(
            P(None, ("sp", "tp"), None),
            P(),
            P("tp", None),
            P("tp", None),
            P(),
            P(),
            P(),
            P(),
        ),
        out_specs=(P("tp", "sp", None), P("tp", "sp", None), P("tp", None)),
        check_vma=False,
    )
```

```python
import functools

import jax
import jax.numpy as jnp
from jax import lax
from jax.experimental import pallas as pl
from jax.experimental.pallas import tpu as pltpu
from jax.sharding import PartitionSpec as P

NORM_EPS = 1e-06
MESH = pl.DeviceIdType.MESH
CORES = 2
SUBLANES = 16


def root_norm(values, scaling):
    inverse = lax.rsqrt(jnp.mean(values * values, axis=-1, keepdims=True) + NORM_EPS)
    return values * inverse * scaling


def remote(src, dst, send, recv, sp, tp):
    return pltpu.make_async_remote_copy(
        src_ref=src, dst_ref=dst, send_sem=send, recv_sem=recv, device_id=(sp, tp), device_id_type=MESH
    )


def kernel(
    dims,
    tok_hbm, gain_ref, wk_hbm, wv_hbm, kgain_ref, query_ref, qgain_ref, bias_ref,
    krecv, vrecv, read_ref,
    tok, normed, wbuf, kvbuf, parts, qall, query,
    tok_sem, own_sem, p1_send, p1_recv, p2_send, p2_recv, p3_send, p3_recv,
    a_send, a_recv, mine_sem, f_send, f_recv,
):
    nsp, ntp, heads, q, group_rows, per_group = dims
    sp, tp = lax.axis_index("sp"), lax.axis_index("tp")
    nz = ntp // CORES
    z, c = tp // CORES, tp % CORES
    partner = z * CORES + (1 - c)
    base, i = (sp // q) * q, sp % q
    seqs, tok_seq, width = tok.shape
    rows = wk_hbm.shape[0]
    part = rows // q
    hd = krecv.shape[2]
    span = ntp * tok_seq
    tp_head = ntp // heads
    half = heads // 2

    def head_at(zc, j):
        home = (zc * CORES) // tp_head
        side = (home // half + (1 if j < half else 0)) % 2
        return side * half + (home % half + (half - 1 - j % half)) % half

    chunks = 2 * heads

    def chunk(zc, m):
        return m // heads, head_at(zc, m % heads)

    fetch = pltpu.make_async_copy(tok_hbm, tok, tok_sem)
    own = []
    for m in range(chunks):
        n, h = chunk(z, m)
        cols = pl.ds(pl.multiple_of(h * hd, hd), hd)
        copy = pltpu.make_async_copy(
            (wk_hbm, wv_hbm)[n].at[:, cols], wbuf.at[n, h, z, c], own_sem.at[m]
        )
        copy.start()
        own.append(copy)
    fetch.start()

    barrier = pltpu.get_barrier_semaphore()
    for d in range(1, ntp):
        pl.semaphore_signal(barrier, inc=1, device_id=(sp, (tp + d) % ntp), device_id_type=MESH)
    for d in range(1, nsp):
        pl.semaphore_signal(barrier, inc=1, device_id=((sp + d) % nsp, tp), device_id_type=MESH)
    for copy in own:
        copy.wait()
    pl.semaphore_wait(barrier, ntp + nsp - 2)

    mine = pl.ds(pl.multiple_of(i * part, part), part)
    sends = []

    for m in range(chunks):
        for d in range(1, nz):
            zt = (z + d) % nz
            n, h = chunk(zt, m)
            block = wbuf.at[n, h, z, c, mine]
            copy = remote(block, block, p1_send.at[m, d], p1_recv.at[m, z], sp, zt * CORES + c)
            copy.start()
            sends.append(copy)

    fetch.wait()
    step_rows = SUBLANES
    per_seq = tok_seq // step_rows

    def norm_rows(n, carry):
        s, at = n // per_seq, pl.ds(pl.multiple_of((n % per_seq) * step_rows, step_rows), step_rows)
        values = tok[s, at].astype(jnp.float32)
        normed[s, at] = root_norm(values, gain_ref[...]).astype(jnp.bfloat16)
        return carry

    lax.fori_loop(0, seqs * per_seq, norm_rows, 0)

    count = query_ref.shape[1] // hd
    for k in range(count):
        values = query_ref[:, k * hd : (k + 1) * hd].astype(jnp.float32)
        qall[k] = root_norm(values, qgain_ref[...])
    group = tp // tp_head
    start = (tp % tp_head) * group_rows
    lines = query.shape[0]
    query[...] = jnp.zeros_like(query)
    for r in range(group_rows):
        for k in range(per_group):
            query[pl.ds(r * per_group + k, 1)] = qall[group * per_group + k, pl.ds(start + r, 1)]
    lanes = lax.broadcasted_iota(jnp.int32, (lines, count), 1)
    which = group * per_group + lax.broadcasted_iota(jnp.int32, (lines, count), 0) % per_group
    bias = jnp.sum(jnp.where(lanes == which, bias_ref[...], 0.0), axis=1, keepdims=True)

    def spread(m):
        n, h = chunk(z, m)
        for d in range(1, nz):
            zs = (z + nz - d) % nz
            block = wbuf.at[n, h, zs, c, mine]
            remote(block, block, p1_send.at[m, d], p1_recv.at[m, zs], sp, zs * CORES + c).wait_recv()
            for e in range(1, q):
                copy = remote(
                    block, block, p2_send.at[m, e, d], p2_recv.at[m, i, zs], base + (i + e) % q, tp
                )
                copy.start()
                sends.append(copy)

    def share(m):
        n, h = chunk(z, m)
        for d in range(1, nz):
            zs = (z + nz - d) % nz
            for e in range(1, q):
                source = (i + e) % q
                block = wbuf.at[n, h, zs, c, pl.ds(pl.multiple_of(source * part, part), part)]
                remote(
                    block, block, p2_send.at[m, e, d], p2_recv.at[m, source, zs], base + source, tp
                ).wait_recv()
        block = wbuf.at[n, h, :, c]
        copy = remote(block, block, p3_send.at[m], p3_recv.at[m], sp, partner)
        copy.start()
        sends.append(copy)

    tile = seqs // 2

    def project(m):
        n, h = chunk(z, m)
        block = wbuf.at[n, h, :, 1 - c]
        remote(block, block, p3_send.at[m], p3_recv.at[m], sp, partner).wait_recv()

        def rows_of(k, carry):
            at = pl.ds(k * tile, tile)
            out = jnp.dot(
                normed[at].reshape(tile * tok_seq, width),
                wbuf[n, h].reshape(width, hd),
                preferred_element_type=jnp.float32,
            )
            if n == 0:
                out = root_norm(out, kgain_ref[...])
            kvbuf[n, h, at] = out.astype(jnp.bfloat16).reshape(tile, tok_seq, hd)
            return carry

        lax.fori_loop(0, seqs // tile, rows_of, 0)

    here = pl.ds(pl.multiple_of(tp * tok_seq, tok_seq), tok_seq)
    landing = (krecv, vrecv)

    def deliver(m):
        n, h = chunk(z, m)
        for u in range(tp_head):
            target = h * tp_head + u
            block = kvbuf.at[n, h, pl.ds(u * group_rows, group_rows)]
            copy = remote(
                block, landing[n].at[:, here], a_send.at[n, target], a_recv.at[n, tp], sp, target
            )
            if m % heads < heads - 1:
                copy.start()
            else:

                @pl.when(target != tp)
                def _(copy=copy):
                    copy.start()

                @pl.when(target == tp)
                def _(block=block):
                    pltpu.make_async_copy(block, landing[n].at[:, here], mine_sem.at[n]).start()

    first = pl.ds(0, group_rows)

    def arrived(n):
        block = kvbuf.at[n, 0, first]
        pltpu.make_async_copy(block, landing[n].at[:, here], mine_sem.at[n]).wait()
        for d in range(1, ntp):
            source = (tp + d) % ntp
            at = pl.ds(pl.multiple_of(source * tok_seq, tok_seq), tok_seq)
            remote(
                block, landing[n].at[:, at], a_send.at[n, source], a_recv.at[n, source], sp, source
            ).wait_recv()

    spread(0)
    for m in range(chunks):
        if m + 1 < chunks:
            spread(m + 1)
        share(m)
        project(m)
        deliver(m)
    arrived(0)

    line = lax.broadcasted_iota(jnp.int32, (lines, 1), 0) // per_group
    raw = jnp.zeros((lines, span), jnp.float32)
    for r in range(group_rows):
        dots = lax.dot_general(
            query[...].astype(jnp.bfloat16), krecv[r], (((1,), (1,)), ((), ())), preferred_element_type=jnp.float32
        )
        raw = jnp.where(line == r, dots, raw)
    scores = raw * hd ** (-0.5) + bias
    soft = jnp.log1p(jnp.exp(-jnp.abs(scores)))
    keep = -jnp.maximum(scores, 0.0) - soft
    take = jnp.minimum(scores, 0.0) - soft
    place = lax.broadcasted_iota(jnp.int32, (lines, span), 1)
    total = keep
    reach = 1
    while reach < span:
        moved = pltpu.roll(total, span - reach, 1)
        total = total + jnp.where(place < span - reach, moved, 0.0)
        reach *= 2
    weights = jnp.exp(take + (total - keep)).astype(jnp.bfloat16)
    arrived(1)
    value = jnp.zeros((lines, hd), jnp.float32)
    for r in range(group_rows):
        dots = jnp.dot(weights, vrecv[r], preferred_element_type=jnp.float32)
        value = jnp.where(line == r, dots, value)
    parts[sp, :, :hd] = value
    parts[sp, :, hd:] = jnp.broadcast_to(total[:, :1], (lines, hd))
    for d in range(1, nsp):
        copy = remote(
            parts.at[sp], parts.at[sp], f_send.at[d], f_recv.at[sp], (sp + d) % nsp, tp
        )
        copy.start()
        sends.append(copy)
    for d in range(1, nsp):
        source = (sp + d) % nsp
        remote(parts.at[source], parts.at[source], f_send.at[d], f_recv.at[source], source, tp).wait_recv()
    result = jnp.zeros((lines, hd), jnp.float32)
    later = jnp.zeros((lines, hd), jnp.float32)
    for n in reversed(range(nsp)):
        result = result + jnp.exp(later) * parts[n, :, :hd]
        later = later + parts[n, :, hd:]
    for r in range(group_rows):
        for k in range(per_group):
            at = r * per_group + k
            read_ref[r : r + 1, k * hd : (k + 1) * hd] = result[at : at + 1]

    for copy in sends:
        copy.wait_send()
    for d in range(1, ntp):
        target = (tp + d) % ntp
        for n in range(2):
            remote(
                kvbuf.at[n, 0, first], landing[n].at[:, here], a_send.at[n, target], a_recv.at[n, tp], sp, target
            ).wait_send()


def shards(sizes, tokens, in_gain, w_key, w_value, k_gain, new_query, q_gain, stick_bias):
    nsp, ntp = sizes
    seqs, tok_seq, width = tokens.shape
    rows, kv_width = w_key.shape
    hd = k_gain.shape[0]
    heads = kv_width // hd
    per_group = stick_bias.shape[0] // heads
    group_rows = heads * seqs // ntp
    used = group_rows * per_group
    lines = -(-used // 8) * 8
    nz = ntp // CORES
    q = min(nsp, rows // SUBLANES)
    span = ntp * tok_seq
    dma = pltpu.SemaphoreType.DMA
    hbm = pl.BlockSpec(memory_space=pltpu.HBM)
    vmem = pl.BlockSpec(memory_space=pltpu.VMEM)
    cache = ((group_rows, span, hd), jnp.bfloat16)
    read = ((group_rows, per_group * hd), jnp.float32)
    chunks = 2 * heads
    return pl.pallas_call(
        functools.partial(kernel, (nsp, ntp, heads, q, group_rows, per_group)),
        out_shape=(pltpu.VMEM(*cache), pltpu.VMEM(*cache), pltpu.VMEM(*read)),
        in_specs=[hbm, vmem, hbm, hbm, vmem, vmem, vmem, vmem],
        out_specs=(vmem, vmem, vmem),
        scratch_shapes=[
            pltpu.VMEM((seqs, tok_seq, width), jnp.bfloat16),
            pltpu.VMEM((seqs, tok_seq, width), jnp.bfloat16),
            pltpu.VMEM((2, heads, nz, CORES, rows, hd), jnp.bfloat16),
            pltpu.VMEM((2, heads, seqs, tok_seq, hd), jnp.bfloat16),
            pltpu.VMEM((nsp, lines, 2 * hd), jnp.float32),
            pltpu.VMEM((heads * per_group, seqs, hd), jnp.float32),
            pltpu.VMEM((lines, hd), jnp.float32),
            dma,
            dma((chunks,)),
            dma((chunks, nz)),
            dma((chunks, nz)),
            dma((chunks, q, nz)),
            dma((chunks, q, nz)),
            dma((chunks,)),
            dma((chunks,)),
            dma((2, ntp)),
            dma((2, ntp)),
            dma((2,)),
            dma((nsp,)),
            dma((nsp,)),
        ],
        compiler_params=pltpu.CompilerParams(
            collective_id=0, has_side_effects=True, vmem_limit_bytes=62 * 1024 * 1024
        ),
    )(
        tokens,
        in_gain.reshape(1, width),
        w_key,
        w_value,
        k_gain.reshape(1, hd),
        new_query,
        q_gain.reshape(1, hd),
        stick_bias.reshape(1, heads * per_group),
    )

def solution(mesh):
    return jax.shard_map(
        functools.partial(shards, (mesh.shape["sp"], mesh.shape["tp"])),
        mesh=mesh,
        in_specs=(
            P(None, ("sp", "tp"), None),
            P(),
            P("tp", None),
            P("tp", None),
            P(),
            P(),
            P(),
            P(),
        ),
        out_specs=(P("tp", "sp", None), P("tp", "sp", None), P("tp", None)),
        check_vma=False,
    )
```

```python
import functools

import jax
import jax.numpy as jnp
from jax import lax
from jax.experimental import pallas as pl
from jax.experimental.pallas import tpu as pltpu
from jax.sharding import PartitionSpec as P

NORM_EPS = 1e-06
MESH = pl.DeviceIdType.MESH
CORES = 2
SUBLANES = 16


def root_norm(values, scaling):
    inverse = lax.rsqrt(jnp.mean(values * values, axis=-1, keepdims=True) + NORM_EPS)
    return values * inverse * scaling


def remote(src, dst, send, recv, sp, tp):
    return pltpu.make_async_remote_copy(
        src_ref=src, dst_ref=dst, send_sem=send, recv_sem=recv, device_id=(sp, tp), device_id_type=MESH
    )


def kernel(
    dims,
    tok_hbm, gain_ref, wk_hbm, wv_hbm, kgain_ref, query_ref, qgain_ref, bias_ref,
    krecv, vrecv, read_ref,
    tok, normed, wbuf, kvbuf, parts, qall, query,
    tok_sem, own_sem, p1_send, p1_recv, p2_send, p2_recv, p3_send, p3_recv,
    a_send, a_recv, mine_sem, f_send, f_recv,
):
    nsp, ntp, heads, q, group_rows, per_group = dims
    sp, tp = lax.axis_index("sp"), lax.axis_index("tp")
    nz = ntp // CORES
    z, c = tp // CORES, tp % CORES
    partner = z * CORES + (1 - c)
    base, i = (sp // q) * q, sp % q
    seqs, tok_seq, width = tok.shape
    rows = wk_hbm.shape[0]
    part = rows // q
    hd = krecv.shape[2]
    span = ntp * tok_seq
    tp_head = ntp // heads
    half = heads // 2

    def head_at(zc, j):
        home = (zc * CORES) // tp_head
        side = (home // half + (1 if j < half else 0)) % 2
        return side * half + (home % half + (half - 1 - j % half)) % half

    chunks = 2 * heads

    def chunk(zc, m):
        return m // heads, head_at(zc, m % heads)

    fetch = pltpu.make_async_copy(tok_hbm, tok, tok_sem)
    own = []
    for m in range(chunks):
        n, h = chunk(z, m)
        cols = pl.ds(pl.multiple_of(h * hd, hd), hd)
        copy = pltpu.make_async_copy(
            (wk_hbm, wv_hbm)[n].at[:, cols], wbuf.at[n, h, z, c], own_sem.at[m]
        )
        copy.start()
        own.append(copy)
    fetch.start()

    barrier = pltpu.get_barrier_semaphore()
    for d in range(1, ntp):
        pl.semaphore_signal(barrier, inc=1, device_id=(sp, (tp + d) % ntp), device_id_type=MESH)
    for d in range(1, nsp):
        pl.semaphore_signal(barrier, inc=1, device_id=((sp + d) % nsp, tp), device_id_type=MESH)
    pl.semaphore_wait(barrier, ntp + nsp - 2)

    mine = pl.ds(pl.multiple_of(i * part, part), part)
    sends = []

    for m in range(chunks):
        if m % heads == 0:
            for copy in own[m : m + heads]:
                copy.wait()
        for d in range(1, nz):
            zt = (z + d) % nz
            n, h = chunk(zt, m)
            block = wbuf.at[n, h, z, c, mine]
            copy = remote(block, block, p1_send.at[m, d], p1_recv.at[m, z], sp, zt * CORES + c)
            copy.start()
            sends.append(copy)

    fetch.wait()
    step_rows = SUBLANES
    per_seq = tok_seq // step_rows

    def norm_rows(n, carry):
        s, at = n // per_seq, pl.ds(pl.multiple_of((n % per_seq) * step_rows, step_rows), step_rows)
        values = tok[s, at].astype(jnp.float32)
        inverse = lax.rsqrt(jnp.mean(values * values, axis=-1, keepdims=True) + NORM_EPS)
        values = tok[s, at].astype(jnp.float32)
        normed[s, at] = (values * inverse * gain_ref[...]).astype(jnp.bfloat16)
        return carry

    def norm_share(n, shares):
        steps = seqs * per_seq
        lax.fori_loop(steps * n // shares, steps * (n + 1) // shares, norm_rows, 0, unroll=4)

    count = query_ref.shape[1] // hd
    for k in range(count):
        values = query_ref[:, k * hd : (k + 1) * hd].astype(jnp.float32)
        qall[k] = root_norm(values, qgain_ref[...])
    group = tp // tp_head
    start = (tp % tp_head) * group_rows
    lines = query.shape[0]
    query[...] = jnp.zeros_like(query)
    for r in range(group_rows):
        for k in range(per_group):
            query[pl.ds(r * per_group + k, 1)] = qall[group * per_group + k, pl.ds(start + r, 1)]
    lanes = lax.broadcasted_iota(jnp.int32, (lines, count), 1)
    which = group * per_group + lax.broadcasted_iota(jnp.int32, (lines, count), 0) % per_group
    bias = jnp.sum(jnp.where(lanes == which, bias_ref[...], 0.0), axis=1, keepdims=True)

    def spread(m):
        n, h = chunk(z, m)
        for d in range(1, nz):
            zs = (z + nz - d) % nz
            block = wbuf.at[n, h, zs, c, mine]
            remote(block, block, p1_send.at[m, d], p1_recv.at[m, zs], sp, zs * CORES + c).wait_recv()
            for e in range(1, q):
                copy = remote(
                    block, block, p2_send.at[m, e, d], p2_recv.at[m, i, zs], base + (i + e) % q, tp
                )
                copy.start()
                sends.append(copy)

    def share(m):
        n, h = chunk(z, m)
        for d in range(1, nz):
            zs = (z + nz - d) % nz
            for e in range(1, q):
                source = (i + e) % q
                block = wbuf.at[n, h, zs, c, pl.ds(pl.multiple_of(source * part, part), part)]
                remote(
                    block, block, p2_send.at[m, e, d], p2_recv.at[m, source, zs], base + source, tp
                ).wait_recv()
        block = wbuf.at[n, h, :, c]
        copy = remote(block, block, p3_send.at[m], p3_recv.at[m], sp, partner)
        copy.start()
        sends.append(copy)

    tile = max(seqs // 2, group_rows)

    def project(m):
        n, h = chunk(z, m)
        block = wbuf.at[n, h, :, 1 - c]
        remote(block, block, p3_send.at[m], p3_recv.at[m], sp, partner).wait_recv()

        for k in range(seqs // tile):
            at = pl.ds(k * tile, tile)
            out = jnp.dot(
                normed[at].reshape(tile * tok_seq, width),
                wbuf[n, h].reshape(width, hd),
                preferred_element_type=jnp.float32,
            )
            if n == 0:
                out = root_norm(out, kgain_ref[...])
            kvbuf[n, h, at] = out.astype(jnp.bfloat16).reshape(tile, tok_seq, hd)
            per_tile = tile // group_rows
            deliver(m, range(k * per_tile, (k + 1) * per_tile))

    here = pl.ds(pl.multiple_of(tp * tok_seq, tok_seq), tok_seq)
    landing = (krecv, vrecv)

    def deliver(m, pieces):
        n, h = chunk(z, m)
        for u in pieces:
            target = h * tp_head + u
            block = kvbuf.at[n, h, pl.ds(u * group_rows, group_rows)]
            copy = remote(
                block, landing[n].at[:, here], a_send.at[n, target], a_recv.at[n, tp], sp, target
            )
            if m % heads < heads - 1:
                copy.start()
            else:

                @pl.when(target != tp)
                def _(copy=copy):
                    copy.start()

                @pl.when(target == tp)
                def _(block=block):
                    pltpu.make_async_copy(block, landing[n].at[:, here], mine_sem.at[n]).start()

    first = pl.ds(0, group_rows)

    def arrived(n):
        block = kvbuf.at[n, 0, first]
        pltpu.make_async_copy(block, landing[n].at[:, here], mine_sem.at[n]).wait()
        for d in range(1, ntp):
            source = (tp + d) % ntp
            at = pl.ds(pl.multiple_of(source * tok_seq, tok_seq), tok_seq)
            remote(
                block, landing[n].at[:, at], a_send.at[n, source], a_recv.at[n, source], sp, source
            ).wait_recv()

    norm_share(0, 3)
    spread(0)
    norm_share(1, 3)
    for m in range(chunks):
        if m + 1 < chunks:
            spread(m + 1)
        share(m)
        if m == 0:
            norm_share(2, 3)
        project(m)
    arrived(0)

    line = lax.broadcasted_iota(jnp.int32, (lines, 1), 0) // per_group
    raw = jnp.zeros((lines, span), jnp.float32)
    for r in range(group_rows):
        dots = lax.dot_general(
            query[...].astype(jnp.bfloat16), krecv[r], (((1,), (1,)), ((), ())), preferred_element_type=jnp.float32
        )
        raw = jnp.where(line == r, dots, raw)
    scores = raw * hd ** (-0.5) + bias
    soft = jnp.log1p(jnp.exp(-jnp.abs(scores)))
    keep = -jnp.maximum(scores, 0.0) - soft
    take = jnp.minimum(scores, 0.0) - soft
    place = lax.broadcasted_iota(jnp.int32, (lines, span), 1)
    total = keep
    reach = 1
    while reach < span:
        moved = pltpu.roll(total, span - reach, 1)
        total = total + jnp.where(place < span - reach, moved, 0.0)
        reach *= 2
    weights = jnp.exp(take + (total - keep)).astype(jnp.bfloat16)
    arrived(1)
    value = jnp.zeros((lines, hd), jnp.float32)
    for r in range(group_rows):
        dots = jnp.dot(weights, vrecv[r], preferred_element_type=jnp.float32)
        value = jnp.where(line == r, dots, value)
    parts[sp, :, :hd] = value
    parts[sp, :, hd:] = jnp.broadcast_to(total[:, :1], (lines, hd))
    for d in range(1, nsp):
        copy = remote(
            parts.at[sp], parts.at[sp], f_send.at[d], f_recv.at[sp], (sp + d) % nsp, tp
        )
        copy.start()
        sends.append(copy)
    for d in range(1, nsp):
        source = (sp + d) % nsp
        remote(parts.at[source], parts.at[source], f_send.at[d], f_recv.at[source], source, tp).wait_recv()
    result = jnp.zeros((lines, hd), jnp.float32)
    later = jnp.zeros((lines, hd), jnp.float32)
    for n in reversed(range(nsp)):
        result = result + jnp.exp(later) * parts[n, :, :hd]
        later = later + parts[n, :, hd:]
    for r in range(group_rows):
        for k in range(per_group):
            at = r * per_group + k
            read_ref[r : r + 1, k * hd : (k + 1) * hd] = result[at : at + 1]

    for copy in sends:
        copy.wait_send()
    for d in range(1, ntp):
        target = (tp + d) % ntp
        for n in range(2):
            remote(
                kvbuf.at[n, 0, first], landing[n].at[:, here], a_send.at[n, target], a_recv.at[n, tp], sp, target
            ).wait_send()


def shards(sizes, tokens, in_gain, w_key, w_value, k_gain, new_query, q_gain, stick_bias):
    nsp, ntp = sizes
    seqs, tok_seq, width = tokens.shape
    rows, kv_width = w_key.shape
    hd = k_gain.shape[0]
    heads = kv_width // hd
    per_group = stick_bias.shape[0] // heads
    group_rows = heads * seqs // ntp
    used = group_rows * per_group
    lines = -(-used // 8) * 8
    nz = ntp // CORES
    q = min(nsp, rows // SUBLANES)
    span = ntp * tok_seq
    dma = pltpu.SemaphoreType.DMA
    hbm = pl.BlockSpec(memory_space=pltpu.HBM)
    vmem = pl.BlockSpec(memory_space=pltpu.VMEM)
    cache = ((group_rows, span, hd), jnp.bfloat16)
    read = ((group_rows, per_group * hd), jnp.float32)
    chunks = 2 * heads
    return pl.pallas_call(
        functools.partial(kernel, (nsp, ntp, heads, q, group_rows, per_group)),
        out_shape=(pltpu.VMEM(*cache), pltpu.VMEM(*cache), pltpu.VMEM(*read)),
        in_specs=[hbm, vmem, hbm, hbm, vmem, vmem, vmem, vmem],
        out_specs=(vmem, vmem, vmem),
        scratch_shapes=[
            pltpu.VMEM((seqs, tok_seq, width), jnp.bfloat16),
            pltpu.VMEM((seqs, tok_seq, width), jnp.bfloat16),
            pltpu.VMEM((2, heads, nz, CORES, rows, hd), jnp.bfloat16),
            pltpu.VMEM((2, heads, seqs, tok_seq, hd), jnp.bfloat16),
            pltpu.VMEM((nsp, lines, 2 * hd), jnp.float32),
            pltpu.VMEM((heads * per_group, seqs, hd), jnp.float32),
            pltpu.VMEM((lines, hd), jnp.float32),
            dma,
            dma((chunks,)),
            dma((chunks, nz)),
            dma((chunks, nz)),
            dma((chunks, q, nz)),
            dma((chunks, q, nz)),
            dma((chunks,)),
            dma((chunks,)),
            dma((2, ntp)),
            dma((2, ntp)),
            dma((2,)),
            dma((nsp,)),
            dma((nsp,)),
        ],
        compiler_params=pltpu.CompilerParams(
            collective_id=0, has_side_effects=True, vmem_limit_bytes=62 * 1024 * 1024
        ),
    )(
        tokens,
        in_gain.reshape(1, width),
        w_key,
        w_value,
        k_gain.reshape(1, hd),
        new_query,
        q_gain.reshape(1, hd),
        stick_bias.reshape(1, heads * per_group),
    )


def solution(mesh):
    return jax.shard_map(
        functools.partial(shards, (mesh.shape["sp"], mesh.shape["tp"])),
        mesh=mesh,
        in_specs=(
            P(None, ("sp", "tp"), None),
            P(),
            P("tp", None),
            P("tp", None),
            P(),
            P(),
            P(),
            P(),
        ),
        out_specs=(P("tp", "sp", None), P("tp", "sp", None), P("tp", None)),
        check_vma=False,
    )
```
